32 devices in a mesh: ep: 16 (over z, y, core), tp: 2 (over x).
Axes of the slice: x: 2, y: 2, z: 4, core: 2. Of those that a mesh axis runs over, the one named last changes fastest.
Arguments:
- tokens: bfloat16 [256, 1024], P('ep', 'tp'), may hold values from -12 to 12
- input_window: bfloat16 [256, 3, 512], P('ep', None, 'tp'), may hold values from -6 to 6
- write_window: bfloat16 [256, 3, 256], P('ep', None, 'tp'), may hold values from -6 to 6
- read_window: bfloat16 [256, 3, 256], P('ep', None, 'tp'), may hold values from -6 to 6
- ssm_state: float32 [256, 8, 64, 64], P('ep', 'tp'), may hold values from -6 to 6
- norm_gain: bfloat16 [1024], replicated, may hold values from 0.099609375 to 1.8984375
- proj_gate: bfloat16 [1024, 512], P(None, 'tp'), may hold values from -0.1875 to 0.1875
- proj_input: bfloat16 [1024, 512], P(None, 'tp'), may hold values from -0.1875 to 0.1875
- proj_write: bfloat16 [1024, 256], P(None, 'tp'), may hold values from -0.1875 to 0.1875
- proj_read: bfloat16 [1024, 256], P(None, 'tp'), may hold values from -0.1875 to 0.1875
- proj_step: bfloat16 [1024, 8], replicated, may hold values from -0.1875 to 0.1875
- taps_input: bfloat16 [4, 512], P(None, 'tp'), may hold values from -3 to 3
- taps_write: bfloat16 [4, 256], P(None, 'tp'), may hold values from -3 to 3
- taps_read: bfloat16 [4, 256], P(None, 'tp'), may hold values from -3 to 3
- step_bias: float32 [8], replicated, may hold values from -2.5 to 0.5
- decay_rate: float32 [8], replicated, may hold values from 0.02 to 2
- skip_gain: float32 [8], replicated, may hold values from 0.1 to 1.9
- out_gain: bfloat16 [512], P('tp'), may hold values from 0.099609375 to 1.8984375
- proj_out: bfloat16 [512, 1024], P('tp'), may hold values from -0.25 to 0.25
- ffn_gain: bfloat16 [1024], replicated, may hold values from 0.099609375 to 1.8984375
- expert_ids: int32 [256, 6], P('ep'), may hold values from 0 to 15, all different within a row; in each aligned block of 16 rows (0 to 15, 16 to 31, ...) at most 9 rows name the same one
- expert_weights: float32 [256, 6], P('ep'), may hold values from 0.05 to 1
- expert_gate: bfloat16 [16, 1024, 512], P('ep', None, 'tp'), may hold values from -0.1875 to 0.1875
- expert_up: bfloat16 [16, 1024, 512], P('ep', None, 'tp'), may hold values from -0.1875 to 0.1875
- expert_down: bfloat16 [16, 512, 1024], P('ep', 'tp'), may hold values from -0.25 to 0.25
- dense_gate: bfloat16 [1024, 1024], P(None, 'tp'), may hold values from -0.1875 to 0.1875
- dense_up: bfloat16 [1024, 1024], P(None, 'tp'), may hold values from -0.1875 to 0.1875
- dense_down: bfloat16 [1024, 1024], P(None, 'tp'), may hold values from -0.5 to 0.5
- branch_gate: bfloat16 [1024], replicated, may hold values from -0.1875 to 0.1875
Outputs:
- new_hidden: bfloat16 [256, 1024], P('ep', 'tp')
- new_state: float32 [256, 8, 64, 64], P('ep', 'tp')
- new_input_window: bfloat16 [256, 3, 512], P('ep', None, 'tp')
- new_write_window: bfloat16 [256, 3, 256], P('ep', None, 'tp')
- new_read_window: bfloat16 [256, 3, 256], P('ep', None, 'tp')
The draws below stay inside these ranges and needn't reach their ends.
Inputs may be any that keep to these rules, and one draw needn't show every extreme that they name: `expert_ids`: each row names 6 different experts. Among the 16 rows of one index of ep no expert is named more than 9 times, and in some aligned block an expert is named exactly 9 times.
All inputs are finite; a program needn't handle non-finite values.
Results may differ from the reference program's by a relative error of at most 0.018.
Values may be sent and summed in bfloat16 or wider, within the bound.
A program may use at most 64 MiB of HBM per device.

```python
import math
import jax
import jax.numpy as jnp
import numpy as np
from jax import lax

D = 1024
HEADS = 8
HEAD_DIM = 64
STATE = 64
BC_GROUPS = 4
CONV = 4
EXP_FF = 512
TOPK = 6
DENSE_FF = 1024
SEQ_DEV = 16
BATCH = 256
EXPERTS = 16
CAP = 9
INNER = 512
LATENT = 256
FF_DEV = 256
N_EP = 16
N_TP = 2


def draw_tokens(key, part):
    key_main = jax.random.fold_in(jax.random.fold_in(key, 11), 0)
    columns = 0.5 * jnp.exp(jnp.log(4.0) * jnp.arange(D, dtype=jnp.float32) / (D - 1))
    values = jax.random.normal(key_main, (BATCH, D), jnp.float32) * columns
    return jnp.clip(values, -12.0, 12.0).astype(jnp.bfloat16)


def block_scale(stream_key, shape, pieces, low, largest):
    loudness = 1.0
    for position, blocks in pieces:
        steps = jax.random.uniform(jax.random.fold_in(jax.random.fold_in(stream_key, 6), position), (blocks,), jnp.float32, low / len(pieces), largest / len(pieces))
        loudness = loudness * jnp.repeat(jnp.exp(steps), shape[position] // blocks).reshape((-1,) + (1,) * (len(shape) - 1 - position))
    return loudness


def assign_block(stream_key, own, number, rows, amount, top, most, slope):
    ranking = jax.random.permutation(stream_key, amount)
    packed, common = shares(amount, rows * top, most, slope, True), shares(amount, rows * top, most, slope, False)
    places = jnp.arange(amount)

    def named(tallies, offset_by):
        used = int((tallies > 0).sum())
        fixed = max(1, used // 4)
        passed = fixed + (places - fixed + offset_by * (used - fixed)) % max(1, amount - fixed)
        return jnp.zeros((amount,), jnp.int32).at[ranking[jnp.where(places < fixed, places, passed)]].set(jnp.asarray(tallies, jnp.int32))

    tallies = jnp.where(number % 4 == 0, named(packed, number // 4), named(common, number - number // 4 - 1))
    mixed = jax.random.permutation(jax.random.fold_in(own, 3), amount)
    donor, taker = mixed[0:amount // 2 * 2:2], mixed[1:amount // 2 * 2:2]
    margin = jnp.minimum(tallies[donor] - 1, most - tallies[taker]) // 2
    margin = jnp.where((donor == ranking[0]) | (taker == ranking[0]) | (tallies[taker] == 0), 0, jnp.maximum(margin, 0))
    passed = jax.random.randint(jax.random.fold_in(own, 4), (amount // 2,), 0, 1 << 20) % (margin + 1)
    tallies = tallies.at[donor].add(-passed).at[taker].add(passed)
    members = jnp.searchsorted(jnp.cumsum(tallies), jnp.arange(rows * top), side="right").astype(jnp.int32)
    table = members.reshape(top, rows).T
    table = table[jax.random.permutation(jax.random.fold_in(own, 1), rows)]
    offset_by = jax.random.randint(jax.random.fold_in(own, 2), (rows, 1), 0, top)
    return jnp.take_along_axis(table, (jnp.arange(top)[None, :] + offset_by) % top, axis=1)


def shares(count, total, reach, slope, full):
    portions = [(1 << 20) // math.isqrt(rank ** slope) + 1 for rank in range(1, count + 1)]
    largest = reach if full else min(reach, max(-(-total // count), total * portions[0] // sum(portions)))
    least = 1 if total - largest >= count - 1 else 0
    holding, rest = [largest] + [least] * (count - 1), total - largest - least * (count - 1)
    while rest > 0:
        movable = [i for i in range(1, count) if holding[i] < largest] or [i for i in range(1, count) if holding[i] < reach]
        pool, left = sum([portions[i] for i in movable]), rest
        for i in movable:
            extra = min(reach - holding[i], max(1, left * portions[i] // pool), rest)
            holding[i] = holding[i] + extra
            rest = rest - extra
    return np.array(holding)


def scatter_about(key, extent, deviation, bound, cuts=(), kind=jnp.bfloat16):
    level = block_scale(key, extent, cuts, -0.22, 0.18) if cuts else 1.0
    entries = jax.random.normal(key, extent, jnp.float32) * deviation * level
    return jnp.minimum(jnp.maximum(entries, -bound), bound).astype(kind)


def setup_inputs(seed: int = 0) -> dict:
    key_list = jax.random.split(jax.random.key(seed), 30)
    tokens = draw_tokens(jax.random.fold_in(key_list[29], 71), 0)
    input_window = scatter_about(key_list[1], (BATCH, CONV - 1, INNER), 1.0, 6.0, ((0, 16), (2, 2)))
    write_window = scatter_about(key_list[2], (BATCH, CONV - 1, LATENT), 1.0, 6.0, ((0, 16), (2, 2)))
    read_window = scatter_about(key_list[3], (BATCH, CONV - 1, LATENT), 1.0, 6.0, ((0, 16), (2, 2)))
    ssm_state = scatter_about(key_list[4], (BATCH, HEADS, HEAD_DIM, STATE), 1.0, 6.0, ((0, 16), (1, 2)), jnp.float32)
    norm_gain = jnp.clip(1.0 + 0.18 * jax.random.normal(key_list[5], (D,), jnp.float32), 0.099609375, 1.8984375).astype(jnp.bfloat16)
    proj_gate = scatter_about(key_list[6], (D, INNER), D ** -0.5, 0.1875, ((1, 2),))
    proj_input = scatter_about(key_list[7], (D, INNER), D ** -0.5, 0.1875, ((1, 2),))
    proj_write = scatter_about(key_list[8], (D, LATENT), D ** -0.5, 0.1875, ((1, 2),))
    proj_read = scatter_about(key_list[9], (D, LATENT), D ** -0.5, 0.1875, ((1, 2),))
    proj_step = scatter_about(key_list[10], (D, HEADS), D ** -0.5, 0.1875)
    taps_input = scatter_about(key_list[11], (CONV, INNER), CONV ** -0.5, 3.0, ((1, 2),))
    taps_write = scatter_about(key_list[12], (CONV, LATENT), CONV ** -0.5, 3.0, ((1, 2),))
    taps_read = scatter_about(key_list[13], (CONV, LATENT), CONV ** -0.5, 3.0, ((1, 2),))
    step_bias = jnp.clip(jax.random.uniform(key_list[14], (HEADS,), jnp.float32, -2.5, 0.5), -2.5, 0.5)
    decay_rate = jnp.clip(jnp.exp(jax.random.uniform(key_list[15], (HEADS,), jnp.float32, math.log(0.02), math.log(2.0))), 0.02, 2.0)
    skip_gain = jnp.clip(1.0 + 0.18 * jax.random.normal(key_list[16], (HEADS,), jnp.float32), 0.1, 1.9)
    out_gain = jnp.clip(1.0 + 0.18 * jax.random.normal(key_list[17], (INNER,), jnp.float32), 0.099609375, 1.8984375).astype(jnp.bfloat16)
    proj_out = scatter_about(key_list[18], (INNER, D), INNER ** -0.5, 0.25, ((0, 2),))
    ffn_gain = jnp.clip(1.0 + 0.18 * jax.random.normal(key_list[19], (D,), jnp.float32), 0.099609375, 1.8984375).astype(jnp.bfloat16)
    expert_ids_keys = jax.random.split(jax.random.fold_in(key_list[20], 1), BATCH // SEQ_DEV)
    expert_ids_turns = jax.random.permutation(jax.random.fold_in(key_list[20], 3), BATCH // SEQ_DEV)
    expert_ids = jax.vmap(lambda own, number: assign_block(jax.random.fold_in(key_list[20], 2), own, number, SEQ_DEV, EXPERTS, TOPK, CAP, 2))(expert_ids_keys, expert_ids_turns).reshape((BATCH, TOPK))
    expert_weights = jnp.clip(jnp.exp(math.log(1.0) - 2.9957323 * jax.random.uniform(key_list[21], (BATCH, TOPK), jnp.float32) ** block_scale(key_list[21], (BATCH, TOPK), ((0, 16),), -0.2, 0.2)), 0.05, 1.0)
    expert_gate = scatter_about(key_list[22], (EXPERTS, D, EXP_FF), D ** -0.5, 0.1875, ((0, 16), (2, 2)))
    expert_up = scatter_about(key_list[23], (EXPERTS, D, EXP_FF), D ** -0.5, 0.1875, ((0, 16), (2, 2)))
    expert_down = scatter_about(key_list[24], (EXPERTS, EXP_FF, D), EXP_FF ** -0.5, 0.25, ((0, 16), (1, 2)))
    dense_gate = scatter_about(key_list[25], (D, DENSE_FF), D ** -0.5, 0.1875, ((1, 2),))
    dense_up = scatter_about(key_list[26], (D, DENSE_FF), D ** -0.5, 0.1875, ((1, 2),))
    dense_down = scatter_about(key_list[27], (D, DENSE_FF), (DENSE_FF // 8) ** -0.5, 0.5, ((1, 2),))
    branch_gate = scatter_about(key_list[28], (D,), D ** -0.5, 0.1875)
    return {"tokens": tokens, "input_window": input_window, "write_window": write_window, "read_window": read_window, "ssm_state": ssm_state, "norm_gain": norm_gain, "proj_gate": proj_gate, "proj_input": proj_input, "proj_write": proj_write, "proj_read": proj_read, "proj_step": proj_step, "taps_input": taps_input, "taps_write": taps_write, "taps_read": taps_read, "step_bias": step_bias, "decay_rate": decay_rate, "skip_gain": skip_gain, "out_gain": out_gain, "proj_out": proj_out, "ffn_gain": ffn_gain, "expert_ids": expert_ids, "expert_weights": expert_weights, "expert_gate": expert_gate, "expert_up": expert_up, "expert_down": expert_down, "dense_gate": dense_gate, "dense_up": dense_up, "dense_down": dense_down, "branch_gate": branch_gate}


EPS = 1e-06

def rms_rows(values, gain):
    widened = values.astype(jnp.float32)
    scale = lax.rsqrt(lax.optimization_barrier(jnp.mean(widened * widened, axis=-1, keepdims=True)) + EPS)
    return widened * scale * gain.astype(jnp.float32)

def short_conv(window, newest, taps):
    stacked = jnp.concatenate([window, newest[:, None, :]], axis=1)
    mixed = lax.optimization_barrier(jnp.sum(stacked.astype(jnp.float32) * taps.astype(jnp.float32)[None], axis=1))
    return (jax.nn.silu(mixed), stacked[:, 1:, :])

def round_trip(values):
    return lax.optimization_barrier(values.astype(jnp.bfloat16)).astype(jnp.float32)

def routed_outputs(normed_ffn, expert_ids, expert_gate, expert_up, expert_down):
    row_count = normed_ffn.shape[0]
    flat_ids = expert_ids.reshape(-1).astype(jnp.int32)
    order = jnp.argsort(flat_ids, stable=True).astype(jnp.int32)
    counts = lax.optimization_barrier(jnp.sum((flat_ids[:, None] == jnp.arange(EXPERTS, dtype=jnp.int32)[None, :]).astype(jnp.int32), axis=0))
    starts = (jnp.cumsum(counts) - counts).astype(jnp.int32)
    most = N_EP * CAP
    padded = jnp.concatenate([order, jnp.zeros((most,), jnp.int32)])
    slot_iota = jnp.arange(most, dtype=jnp.int32)

    def visit(totals, expert):
        picked = lax.dynamic_slice(padded, (starts[expert],), (most,))
        live = slot_iota < counts[expert]
        inputs = normed_ffn[picked // TOPK]
        gate_part = jnp.dot(inputs, expert_gate[expert], preferred_element_type=jnp.float32)
        up_part = jnp.dot(inputs, expert_up[expert], preferred_element_type=jnp.float32)
        hidden = (jax.nn.silu(gate_part) * up_part).astype(jnp.bfloat16)
        blocks = jnp.einsum('mtf,tfd->mtd', hidden.reshape(most, N_TP, FF_DEV).astype(jnp.float32), expert_down[expert].reshape(N_TP, FF_DEV, D).astype(jnp.float32))
        summed = lax.optimization_barrier(jnp.sum(round_trip(blocks), axis=1))
        result = round_trip(summed)
        return (totals.at[picked].add(jnp.where(live[:, None], result, 0.0)), None)
    start_totals = jnp.zeros((row_count * TOPK, D), jnp.float32)
    totals = lax.scan(visit, start_totals, jnp.arange(EXPERTS, dtype=jnp.int32))[0]
    return totals.reshape(row_count, TOPK, D)

def reference(tokens, input_window, write_window, read_window, ssm_state, norm_gain, proj_gate, proj_input, proj_write, proj_read, proj_step, taps_input, taps_write, taps_read, step_bias, decay_rate, skip_gain, out_gain, proj_out, ffn_gain, expert_ids, expert_weights, expert_gate, expert_up, expert_down, dense_gate, dense_up, dense_down, branch_gate):
    row_count = tokens.shape[0]
    normed = rms_rows(tokens, norm_gain).astype(jnp.bfloat16)
    gate_rows = jnp.dot(normed, proj_gate, preferred_element_type=jnp.float32).astype(jnp.bfloat16)
    input_rows = jnp.dot(normed, proj_input, preferred_element_type=jnp.float32).astype(jnp.bfloat16)
    write_rows = jnp.dot(normed, proj_write, preferred_element_type=jnp.float32).astype(jnp.bfloat16)
    read_rows = jnp.dot(normed, proj_read, preferred_element_type=jnp.float32).astype(jnp.bfloat16)
    step_raw = jnp.dot(normed, proj_step, preferred_element_type=jnp.float32)
    input_conv, new_input_window = short_conv(input_window, input_rows, taps_input)
    write_conv, new_write_window = short_conv(write_window, write_rows, taps_write)
    read_conv, new_read_window = short_conv(read_window, read_rows, taps_read)
    step_size = jax.nn.softplus(step_raw + step_bias.astype(jnp.float32))
    decay = jnp.exp(-step_size * decay_rate.astype(jnp.float32))
    heads_input = input_conv.reshape(row_count, HEADS, HEAD_DIM)
    per_group = HEADS // BC_GROUPS
    write_heads = jnp.repeat(write_conv.reshape(row_count, BC_GROUPS, STATE), per_group, axis=1)
    read_heads = jnp.repeat(read_conv.reshape(row_count, BC_GROUPS, STATE), per_group, axis=1)
    new_state = decay[:, :, None, None] * ssm_state + (step_size[:, :, None] * heads_input)[:, :, :, None] * write_heads[:, :, None, :]
    readout = jnp.einsum('bhpn,bhn->bhp', new_state, read_heads, precision=lax.Precision.HIGHEST)
    readout = readout + skip_gain.astype(jnp.float32)[None, :, None] * heads_input
    gated = readout.reshape(row_count, INNER) * jax.nn.silu(gate_rows.astype(jnp.float32))
    grouped = gated.reshape(row_count, BC_GROUPS, INNER // BC_GROUPS)
    grouped = grouped * lax.rsqrt(lax.optimization_barrier(jnp.mean(grouped * grouped, axis=-1, keepdims=True)) + EPS)
    mixer_rows = (grouped.reshape(row_count, INNER) * out_gain.astype(jnp.float32)).astype(jnp.bfloat16)
    blocks = jnp.einsum('btk,tkd->btd', mixer_rows.reshape(row_count, N_TP, INNER // N_TP).astype(jnp.float32), proj_out.reshape(N_TP, INNER // N_TP, D).astype(jnp.float32))
    mixed = lax.optimization_barrier(jnp.sum(round_trip(blocks), axis=1))
    hidden_rows = (tokens.astype(jnp.float32) + mixed).astype(jnp.bfloat16)
    normed_ffn = rms_rows(hidden_rows, ffn_gain).astype(jnp.bfloat16)
    routed = routed_outputs(normed_ffn, expert_ids, expert_gate, expert_up, expert_down)
    expert_sum = lax.optimization_barrier(jnp.sum(expert_weights.astype(jnp.float32)[:, :, None] * routed, axis=1))
    dense_gate_part = jnp.dot(normed_ffn, dense_gate, preferred_element_type=jnp.float32)
    dense_up_part = jnp.dot(normed_ffn, dense_up, preferred_element_type=jnp.float32)
    dense_hidden = (jax.nn.silu(dense_gate_part) * dense_up_part).astype(jnp.bfloat16)
    dense_sum = lax.dot_general(dense_hidden, dense_down, (((1,), (1,)), ((), ())), preferred_element_type=jnp.float32)
    branch = jax.nn.sigmoid(jnp.dot(normed_ffn, branch_gate, preferred_element_type=jnp.float32))
    new_hidden = (hidden_rows.astype(jnp.float32) + expert_sum + branch[:, None] * dense_sum).astype(jnp.bfloat16)
    return (new_hidden, new_state, new_input_window, new_write_window, new_read_window)
```

```python
import functools

import jax
import jax.numpy as jnp
from jax import lax
from jax.experimental import pallas as pl
from jax.experimental.pallas import tpu as pltpu
from jax.sharding import PartitionSpec as P

HEADS = 8
HEAD_DIM = 64
STATE = 64
BC_GROUPS = 4
EPS = 1e-06
LANES = 8

F32 = jnp.float32
BF16 = jnp.bfloat16


def dot(a, b):
    return jnp.dot(a, b, preferred_element_type=F32)


def silu(v):
    return v / (1.0 + jnp.exp(-v))


def remote(src, dst, send, recv, where):
    return pltpu.make_async_remote_copy(
        src_ref=src,
        dst_ref=dst,
        send_sem=send,
        recv_sem=recv,
        device_id=where,
        device_id_type=pl.DeviceIdType.MESH,
    )


def drain(ref, sem):
    pltpu.make_async_copy(ref, ref, sem).wait()


def kernel(
    n_ep,
    n_tp,
    capacity,
    tokens,
    input_window,
    write_window,
    read_window,
    state_hbm,
    gains,
    proj_gate_hbm,
    proj_input_hbm,
    proj_write_hbm,
    proj_read_hbm,
    proj_step,
    taps_input,
    taps_write,
    taps_read,
    step_bias,
    decay_rate,
    skip_gain,
    proj_out_hbm,
    expert_ids,
    expert_weights,
    expert_gate_hbm,
    expert_up_hbm,
    expert_down_hbm,
    dense_gate_hbm,
    dense_up_hbm,
    dense_down_hbm,
    new_hidden,
    new_state_hbm,
    new_input_window,
    new_write_window,
    new_read_window,
    proj_gate,
    proj_input,
    proj_write,
    proj_read,
    proj_out,
    expert_gate,
    expert_up,
    expert_down,
    dense_gate,
    dense_up,
    dense_down,
    state,
    new_state,
    tok_all,
    part_all,
    hid_all,
    send_main,
    recv_main,
    send_extra,
    recv_extra,
    back_main,
    ret_main,
    back_extra,
    ret_extra,
    dense_send,
    dense_recv,
    weight_sems,
    state_sem,
    pair_send,
    pair_recv,
    a2a_send,
    a2a_recv,
):
    ep = lax.axis_index("ep")
    tp = lax.axis_index("tp")
    rows, quarter = tokens.shape
    width = quarter * n_tp
    main = capacity // LANES * LANES
    extra = capacity - main

    barrier = pltpu.get_barrier_semaphore()

    def greet(step, carry):
        for shift in range(n_tp):
            there = {"ep": lax.rem(ep + step, n_ep), "tp": lax.rem(tp + shift, n_tp)}

            def tell():
                pl.semaphore_signal(
                    barrier, inc=1, device_id=there, device_id_type=pl.DeviceIdType.MESH
                )

            if shift == 0:
                pl.when(step > 0)(tell)
            else:
                tell()
        return carry

    lax.fori_loop(0, n_ep, greet, 0)

    pairs = (
        (proj_gate_hbm, proj_gate),
        (proj_input_hbm, proj_input),
        (proj_write_hbm, proj_write),
        (proj_read_hbm, proj_read),
        (state_hbm, state),
        (proj_out_hbm, proj_out),
        (dense_gate_hbm, dense_gate),
        (dense_up_hbm, dense_up),
        (dense_down_hbm, dense_down),
        (expert_gate_hbm, expert_gate),
        (expert_up_hbm, expert_up),
        (expert_down_hbm, expert_down),
    )
    loads = [pltpu.make_async_copy(s, d, weight_sems.at[i]) for i, (s, d) in enumerate(pairs)]
    for load in loads:
        load.start()

    ids = expert_ids[...]
    weights = expert_weights[...]
    expert_lane = lax.broadcasted_iota(jnp.int32, (rows, n_ep), 1)
    hits = jnp.zeros((rows, n_ep), F32)
    scale = jnp.zeros((rows, n_ep), F32)
    for k in range(ids.shape[1]):
        same = ids[:, k : k + 1] == expert_lane
        hits = hits + jnp.where(same, 1.0, 0.0)
        scale = scale + jnp.where(same, weights[:, k : k + 1], 0.0)
    earlier = jnp.where(
        lax.broadcasted_iota(jnp.int32, (rows, rows), 1)
        < lax.broadcasted_iota(jnp.int32, (rows, rows), 0),
        1.0,
        0.0,
    ).astype(BF16)
    place = dot(earlier, hits.astype(BF16))
    scale_hi = scale.astype(BF16)
    scale_lo = (scale - scale_hi.astype(F32)).astype(BF16)
    if main:
        slots = n_ep * main
        slot = lax.broadcasted_iota(jnp.int32, (n_ep, slots), 1).astype(F32)
        owner = jnp.floor((slot + 0.5) / main)
        spread = jnp.where(
            owner == lax.broadcasted_iota(jnp.int32, (n_ep, slots), 0).astype(F32), 1.0, 0.0
        ).astype(BF16)
        lane = lax.broadcasted_iota(jnp.int32, (rows, slots), 1).astype(F32)
        index = lane - main * jnp.floor((lane + 0.5) / main)
        takes = jnp.logical_and(
            dot(hits.astype(BF16), spread) > 0.5, jnp.abs(dot(place.astype(BF16), spread) - index) < 0.5
        )
        chosen = jnp.where(takes, 1.0, 0.0)
        chosen_main = jnp.transpose(chosen).astype(BF16)
        main_hi = (dot(scale_hi, spread) * chosen).astype(BF16)
        main_lo = (dot(scale_lo, spread) * chosen).astype(BF16)
    chosen_extra, extra_hi, extra_lo = [], [], []
    for j in range(extra):
        takes = jnp.where(
            jnp.logical_and(hits > 0.5, jnp.abs(place - (main + j)) < 0.5), 1.0, 0.0
        )
        chosen_extra.append(takes.astype(BF16))
        extra_hi.append((scale_hi.astype(F32) * takes).astype(BF16))
        extra_lo.append((scale_lo.astype(F32) * takes).astype(BF16))

    pl.semaphore_wait(barrier, n_ep * n_tp - 1)

    def exchange(buffer, k):
        copies = []
        for shift in range(1, n_tp):
            copies.append(
                remote(
                    buffer.at[tp],
                    buffer.at[tp],
                    pair_send.at[k, shift],
                    pair_recv.at[k, shift],
                    {"tp": lax.rem(tp + shift, n_tp)},
                )
            )
            copies[-1].start()
        return copies

    tok_all[tp] = tokens[...]
    for copy in exchange(tok_all, 0):
        copy.wait()

    def norm(pieces, row):
        wide = jnp.concatenate(pieces, axis=1)
        factor = lax.rsqrt(jnp.sum(wide * wide, axis=1, keepdims=True) / width + EPS)
        return (wide * factor * gains[row : row + 1, :]).astype(BF16)

    token_parts = [tok_all[t].astype(F32) for t in range(n_tp)]
    normed = norm(token_parts, 0)

    for i in range(4):
        loads[i].wait()
    gate_rows = dot(normed, proj_gate[...]).astype(BF16)
    input_rows = dot(normed, proj_input[...]).astype(BF16)
    write_rows = dot(normed, proj_write[...]).astype(BF16)
    read_rows = dot(normed, proj_read[...]).astype(BF16)
    step_all = dot(normed, proj_step[...])

    def conv(window, newest, taps, result):
        old = window[...].astype(F32)
        lines = [old[:, i, :] for i in range(old.shape[1])] + [newest.astype(F32)]
        tap = taps[...].astype(F32)
        total = lines[0] * tap[0:1, :]
        for i in range(1, len(lines)):
            total = total + lines[i] * tap[i : i + 1, :]
        result[...] = jnp.stack(lines[1:], axis=1).astype(BF16)
        return silu(total)

    input_conv = conv(input_window, input_rows, taps_input, new_input_window)
    write_conv = conv(write_window, write_rows, taps_write, new_write_window)
    read_conv = conv(read_window, read_rows, taps_read, new_read_window)

    heads_dev = state.shape[1]
    groups_dev = write_conv.shape[1] // STATE
    per_group = heads_dev // groups_dev
    head_lane = lax.broadcasted_iota(jnp.int32, step_all.shape, 1)
    loads[4].wait()
    row_lane = lax.broadcasted_iota(jnp.int32, (HEAD_DIM, rows), 1)
    readouts = []
    for h in range(heads_dev):
        at = tp * heads_dev + h
        raw = jnp.sum(jnp.where(head_lane == at, step_all, 0.0), axis=1, keepdims=True)
        biased = raw + step_bias[at]
        size = jnp.maximum(biased, 0.0) + jnp.log1p(jnp.exp(-jnp.abs(biased)))
        decay = jnp.exp(-size * decay_rate[at])
        head_in = input_conv[:, h * HEAD_DIM : (h + 1) * HEAD_DIM]
        scaled = jnp.transpose(size * head_in)
        g = h // per_group
        write = write_conv[:, g * STATE : (g + 1) * STATE]
        read = read_conv[:, g * STATE : (g + 1) * STATE]
        columns = jnp.zeros((HEAD_DIM, rows), F32)
        for b in range(rows):
            fresh = decay[b : b + 1, :] * state[b, h] + scaled[:, b : b + 1] * write[b : b + 1, :]
            new_state[b, h] = fresh
            column = jnp.sum(fresh * read[b : b + 1, :], axis=1, keepdims=True)
            columns = jnp.where(row_lane == b, column, columns)
        readouts.append(jnp.transpose(columns) + skip_gain[at] * head_in)
    keep = pltpu.make_async_copy(new_state, new_state_hbm, state_sem)
    keep.start()
    gated = jnp.concatenate(readouts, axis=1) * silu(gate_rows.astype(F32))
    span = gated.shape[1] // groups_dev
    grouped = []
    for g in range(groups_dev):
        piece = gated[:, g * span : (g + 1) * span]
        grouped.append(
            piece * lax.rsqrt(jnp.mean(piece * piece, axis=1, keepdims=True) + EPS)
        )
    mixer_rows = (jnp.concatenate(grouped, axis=1) * gains[3:4, : gated.shape[1]]).astype(BF16)
    loads[5].wait()
    part_all[tp] = dot(mixer_rows, proj_out[...]).astype(BF16)
    for copy in exchange(part_all, 1):
        copy.wait()

    mixed = part_all[0].astype(F32)
    for t in range(1, n_tp):
        mixed = mixed + part_all[t].astype(F32)
    hidden_parts = []
    for t in range(n_tp):
        part = (token_parts[t] + mixed[:, t * quarter : (t + 1) * quarter]).astype(BF16)
        hid_all[t] = part
        hidden_parts.append(part.astype(F32))
    normed_ffn = norm(hidden_parts, 1)

    if main:
        send_main[...] = dot(chosen_main, normed_ffn).astype(BF16).reshape(send_main.shape)
    for j in range(extra):
        send_extra[j] = dot(jnp.transpose(chosen_extra[j].astype(F32)).astype(BF16), normed_ffn)[
            :, None, :
        ]

    def dispatch(step, carry):
        peer = lax.rem(ep + step, n_ep)
        if main:
            remote(
                send_main.at[peer], recv_main.at[ep], a2a_send.at[0], a2a_recv.at[0], {"ep": peer}
            ).start()
        for j in range(extra):
            remote(
                send_extra.at[j, peer],
                recv_extra.at[j, ep],
                a2a_send.at[1],
                a2a_recv.at[1],
                {"ep": peer},
            ).start()
        return carry

    lax.fori_loop(1, n_ep, dispatch, 0)
    if main:
        pltpu.make_async_copy(send_main.at[ep], recv_main.at[ep], a2a_recv.at[0]).start()
    for j in range(extra):
        pltpu.make_async_copy(send_extra.at[j, ep], recv_extra.at[j, ep], a2a_recv.at[1]).start()

    for i in range(6, 9):
        loads[i].wait()
    dense_hidden = (
        silu(dot(normed_ffn, dense_gate[...])) * dot(normed_ffn, dense_up[...])
    ).astype(BF16)
    for t in range(n_tp):
        dense_send[t] = lax.dot_general(
            dense_hidden,
            dense_down[t * quarter : (t + 1) * quarter, :],
            (((1,), (1,)), ((), ())),
            preferred_element_type=F32,
        ).astype(BF16)
    dense_copies = []
    for shift in range(1, n_tp):
        there = lax.rem(tp + shift, n_tp)
        dense_copies.append(
            remote(
                dense_send.at[there],
                dense_recv.at[tp],
                pair_send.at[2, shift],
                pair_recv.at[2, shift],
                {"tp": there},
            )
        )
        dense_copies[-1].start()
    logit = jnp.sum(normed_ffn.astype(F32) * gains[2:3, :], axis=1, keepdims=True)
    branch = 1.0 / (1.0 + jnp.exp(-logit))

    for i in range(9, 12):
        loads[i].wait()
    arrived = []
    if main:
        drain(recv_main, a2a_recv.at[0])
        arrived.append(recv_main[...].reshape(n_ep * main, width))
    if extra:
        drain(recv_extra, a2a_recv.at[1])
        for j in range(extra):
            arrived.append(recv_extra[j].reshape(n_ep, width).astype(BF16))
    arrived = jnp.concatenate(arrived, axis=0) if len(arrived) > 1 else arrived[0]
    hidden = (silu(dot(arrived, expert_gate[0])) * dot(arrived, expert_up[0])).astype(BF16)
    for t in range(n_tp):
        produced = dot(hidden, expert_down[0, :, t * quarter : (t + 1) * quarter])
        if main:
            back_main[t] = produced[: n_ep * main].astype(BF16).reshape(back_main.shape[1:])
        for j in range(extra):
            start = n_ep * (main + j)
            back_extra[j, t] = produced[start : start + n_ep][:, None, :]

    def give_back(step, carry):
        peer = lax.rem(ep + step, n_ep)
        for shift in range(n_tp):
            there = lax.rem(tp + shift, n_tp)

            def go():
                if main:
                    remote(
                        back_main.at[there, peer],
                        ret_main.at[tp, ep],
                        a2a_send.at[2],
                        a2a_recv.at[2],
                        {"ep": peer, "tp": there},
                    ).start()
                for j in range(extra):
                    remote(
                        back_extra.at[j, there, peer],
                        ret_extra.at[j, tp, ep],
                        a2a_send.at[3],
                        a2a_recv.at[3],
                        {"ep": peer, "tp": there},
                    ).start()

            if shift == 0:
                pl.when(step > 0)(go)
            else:
                go()
        return carry

    lax.fori_loop(0, n_ep, give_back, 0)
    if main:
        pltpu.make_async_copy(back_main.at[tp, ep], ret_main.at[tp, ep], a2a_recv.at[2]).start()
    for j in range(extra):
        pltpu.make_async_copy(
            back_extra.at[j, tp, ep], ret_extra.at[j, tp, ep], a2a_recv.at[3]
        ).start()

    for copy in dense_copies:
        copy.wait()
    dense_sum = dense_send[tp].astype(F32)
    for shift in range(1, n_tp):
        dense_sum = dense_sum + dense_recv[lax.rem(tp + shift, n_tp)].astype(F32)
    total = hid_all[tp].astype(F32) + branch * dense_sum

    if main:
        drain(ret_main, a2a_recv.at[2])
        for t in range(n_tp):
            back = ret_main[t].reshape(n_ep * main, quarter)
            total = total + dot(main_hi, back) + dot(main_lo, back)
    if extra:
        drain(ret_extra, a2a_recv.at[3])
        for j in range(extra):
            for t in range(n_tp):
                back = ret_extra[j, t].reshape(n_ep, quarter).astype(BF16)
                total = total + dot(extra_hi[j], back) + dot(extra_lo[j], back)
    new_hidden[...] = total.astype(BF16)

    def left(step, carry):
        if main:
            drain(send_main.at[0], a2a_send.at[0])
        for j in range(extra):
            drain(send_extra.at[j, 0], a2a_send.at[1])
        return carry

    lax.fori_loop(1, n_ep, left, 0)

    def left_back(step, carry):
        if main:
            drain(back_main.at[0, 0], a2a_send.at[2])
        for j in range(extra):
            drain(back_extra.at[j, 0, 0], a2a_send.at[3])
        return carry

    lax.fori_loop(1, n_ep * n_tp, left_back, 0)
    keep.wait()


def local(
    n_ep,
    n_tp,
    tokens,
    input_window,
    write_window,
    read_window,
    ssm_state,
    norm_gain,
    proj_gate,
    proj_input,
    proj_write,
    proj_read,
    proj_step,
    taps_input,
    taps_write,
    taps_read,
    step_bias,
    decay_rate,
    skip_gain,
    out_gain,
    proj_out,
    ffn_gain,
    expert_ids,
    expert_weights,
    expert_gate,
    expert_up,
    expert_down,
    dense_gate,
    dense_up,
    dense_down,
    branch_gate,
):
    rows, quarter = tokens.shape
    width = norm_gain.shape[0]
    top_count = expert_ids.shape[1]
    capacity = min(rows, max(2, (3 * rows * top_count + 2 * n_ep - 1) // (2 * n_ep)))
    main = capacity // LANES * LANES
    extra = capacity - main
    held = max(main, LANES)
    spare = max(extra, 1)
    gains = jnp.stack(
        [norm_gain, ffn_gain, branch_gate, jnp.pad(out_gain, (0, width - out_gain.shape[0]))]
    ).astype(F32)
    vmem = pl.BlockSpec(memory_space=pltpu.VMEM)
    smem = pl.BlockSpec(memory_space=pltpu.SMEM)
    hbm = pl.BlockSpec(memory_space=pl.ANY)
    streamed = (
        proj_gate,
        proj_input,
        proj_write,
        proj_read,
        proj_out,
        expert_gate,
        expert_up,
        expert_down,
        dense_gate,
        dense_up,
        dense_down,
        ssm_state,
    )
    shape_of = lambda a: jax.ShapeDtypeStruct(a.shape, a.dtype)
    return pl.pallas_call(
        functools.partial(kernel, n_ep, n_tp, capacity),
        out_shape=(
            shape_of(tokens),
            shape_of(ssm_state),
            shape_of(input_window),
            shape_of(write_window),
            shape_of(read_window),
        ),
        in_specs=[vmem] * 4
        + [hbm, vmem]
        + [hbm] * 4
        + [vmem] * 4
        + [smem] * 3
        + [hbm, vmem, vmem]
        + [hbm] * 6,
        out_specs=(vmem, hbm, vmem, vmem, vmem),
        scratch_shapes=[pltpu.VMEM(a.shape, a.dtype) for a in streamed]
        + [
            pltpu.VMEM(ssm_state.shape, F32),
            pltpu.VMEM((n_tp, rows, quarter), BF16),
            pltpu.VMEM((n_tp, rows, width), BF16),
            pltpu.VMEM((n_tp, rows, quarter), BF16),
            pltpu.VMEM((n_ep, held, width), BF16),
            pltpu.VMEM((n_ep, held, width), BF16),
            pltpu.VMEM((spare, n_ep, 1, width), F32),
            pltpu.VMEM((spare, n_ep, 1, width), F32),
            pltpu.VMEM((n_tp, n_ep, held, quarter), BF16),
            pltpu.VMEM((n_tp, n_ep, held, quarter), BF16),
            pltpu.VMEM((spare, n_tp, n_ep, 1, quarter), F32),
            pltpu.VMEM((spare, n_tp, n_ep, 1, quarter), F32),
            pltpu.VMEM((n_tp, rows, quarter), BF16),
            pltpu.VMEM((n_tp, rows, quarter), BF16),
            pltpu.SemaphoreType.DMA((12,)),
            pltpu.SemaphoreType.DMA,
            pltpu.SemaphoreType.DMA((3, n_tp)),
            pltpu.SemaphoreType.DMA((3, n_tp)),
            pltpu.SemaphoreType.DMA((4,)),
            pltpu.SemaphoreType.DMA((4,)),
        ],
        compiler_params=pltpu.CompilerParams(
            collective_id=0, has_side_effects=True, vmem_limit_bytes=60 * 1024 * 1024
        ),
    )(
        tokens,
        input_window,
        write_window,
        read_window,
        ssm_state,
        gains,
        proj_gate,
        proj_input,
        proj_write,
        proj_read,
        proj_step,
        taps_input,
        taps_write,
        taps_read,
        step_bias,
        decay_rate,
        skip_gain,
        proj_out,
        expert_ids,
        expert_weights,
        expert_gate,
        expert_up,
        expert_down,
        dense_gate,
        dense_up,
        dense_down,
    )


def solution(mesh):
    in_specs = (
        P("ep", "tp"),
        P("ep", None, "tp"),
        P("ep", None, "tp"),
        P("ep", None, "tp"),
        P("ep", "tp", None, None),
        P(),
        P(None, "tp"),
        P(None, "tp"),
        P(None, "tp"),
        P(None, "tp"),
        P(),
        P(None, "tp"),
        P(None, "tp"),
        P(None, "tp"),
        P(),
        P(),
        P(),
        P("tp"),
        P("tp", None),
        P(),
        P("ep", None),
        P("ep", None),
        P("ep", None, "tp"),
        P("ep", None, "tp"),
        P("ep", "tp", None),
        P(None, "tp"),
        P(None, "tp"),
        P(None, "tp"),
        P(),
    )
    out_specs = (
        P("ep", "tp"),
        P("ep", "tp", None, None),
        P("ep", None, "tp"),
        P("ep", None, "tp"),
        P("ep", None, "tp"),
    )
    step = functools.partial(local, mesh.shape["ep"], mesh.shape["tp"])
    return jax.shard_map(step, mesh=mesh, in_specs=in_specs, out_specs=out_specs, check_vma=False)
```

```python
import functools

import jax
import jax.numpy as jnp
from jax import lax
from jax.experimental import pallas as pl
from jax.experimental.pallas import tpu as pltpu
from jax.sharding import PartitionSpec as P

HEADS = 8
HEAD_DIM = 64
STATE = 64
BC_GROUPS = 4
EPS = 1e-06
LANES = 8
PIECES = 8

F32 = jnp.float32
BF16 = jnp.bfloat16


def dot(a, b):
    return jnp.dot(a, b, preferred_element_type=F32)


def silu(v):
    return v / (1.0 + jnp.exp(-v))


def remote(src, dst, send, recv, where):
    return pltpu.make_async_remote_copy(
        src_ref=src,
        dst_ref=dst,
        send_sem=send,
        recv_sem=recv,
        device_id=where,
        device_id_type=pl.DeviceIdType.MESH,
    )


def drain(ref, sem):
    pltpu.make_async_copy(ref, ref, sem).wait()


def kernel(
    n_ep,
    n_tp,
    capacity,
    tokens,
    input_window,
    write_window,
    read_window,
    state_hbm,
    norm_gain,
    ffn_gain,
    branch_gate,
    out_gain,
    proj_gate_hbm,
    proj_input_hbm,
    proj_write_hbm,
    proj_read_hbm,
    proj_step,
    taps_input,
    taps_write,
    taps_read,
    step_bias,
    decay_rate,
    skip_gain,
    proj_out_hbm,
    expert_ids,
    expert_weights,
    expert_gate_hbm,
    expert_up_hbm,
    expert_down_hbm,
    dense_gate_hbm,
    dense_up_hbm,
    dense_down_hbm,
    new_hidden,
    new_state_hbm,
    new_input_window,
    new_write_window,
    new_read_window,
    proj_gate,
    proj_input,
    proj_write,
    proj_read,
    proj_out,
    expert_gate,
    expert_up,
    expert_down,
    dense_gate,
    dense_up,
    dense_down,
    state,
    new_state,
    tok_all,
    part_all,
    hid_all,
    send_main,
    recv_main,
    send_extra,
    recv_extra,
    back_main,
    ret_main,
    back_extra,
    ret_extra,
    dense_send,
    dense_recv,
    weight_sems,
    state_sem,
    pair_send,
    pair_recv,
    a2a_send,
    a2a_recv,
):
    ep = lax.axis_index("ep")
    tp = lax.axis_index("tp")
    rows, quarter = tokens.shape
    width = quarter * n_tp
    main = capacity // LANES * LANES
    extra = capacity - main

    barrier = pltpu.get_barrier_semaphore()

    def greet(step, carry):
        for shift in range(n_tp):
            there = {"ep": lax.rem(ep + step, n_ep), "tp": lax.rem(tp + shift, n_tp)}

            def tell():
                pl.semaphore_signal(
                    barrier, inc=1, device_id=there, device_id_type=pl.DeviceIdType.MESH
                )

            if shift == 0:
                pl.when(step > 0)(tell)
            else:
                tell()
        return carry

    lax.fori_loop(0, n_ep, greet, 0)

    pairs = (
        (proj_gate_hbm, proj_gate),
        (proj_input_hbm, proj_input),
        (proj_write_hbm, proj_write),
        (proj_read_hbm, proj_read),
        (state_hbm, state),
        (proj_out_hbm, proj_out),
        (dense_gate_hbm, dense_gate),
        (dense_up_hbm, dense_up),
        (dense_down_hbm, dense_down),
        (expert_gate_hbm, expert_gate),
        (expert_up_hbm, expert_up),
        (expert_down_hbm, expert_down),
    )
    loads = [pltpu.make_async_copy(s, d, weight_sems.at[i]) for i, (s, d) in enumerate(pairs)]
    for load in loads:
        load.start()

    ids = expert_ids[...]
    weights = expert_weights[...]
    expert_row = lax.broadcasted_iota(jnp.int32, (n_ep, rows), 0)
    hits = jnp.zeros((n_ep, rows), F32)
    scale = jnp.zeros((n_ep, rows), F32)
    for k in range(ids.shape[0]):
        same = ids[k : k + 1, :] == expert_row
        hits = hits + jnp.where(same, 1.0, 0.0)
        scale = scale + jnp.where(same, weights[k : k + 1, :], 0.0)
    earlier = jnp.where(
        lax.broadcasted_iota(jnp.int32, (rows, rows), 0)
        < lax.broadcasted_iota(jnp.int32, (rows, rows), 1),
        1.0,
        0.0,
    ).astype(BF16)
    place = dot(hits.astype(BF16), earlier)
    scale_hi = scale.astype(BF16)
    scale_lo = (scale - scale_hi.astype(F32)).astype(BF16)
    if main:
        slots = n_ep * main
        slot = lax.broadcasted_iota(jnp.int32, (slots, n_ep), 0).astype(F32)
        owner = jnp.floor((slot + 0.5) / main)
        spread = jnp.where(
            owner == lax.broadcasted_iota(jnp.int32, (slots, n_ep), 1).astype(F32), 1.0, 0.0
        ).astype(BF16)
        lane = lax.broadcasted_iota(jnp.int32, (slots, rows), 0).astype(F32)
        index = lane - main * jnp.floor((lane + 0.5) / main)
        takes = jnp.logical_and(
            dot(spread, hits.astype(BF16)) > 0.5,
            jnp.abs(dot(spread, place.astype(BF16)) - index) < 0.5,
        )
        chosen = jnp.where(takes, 1.0, 0.0)
        chosen_main = chosen.astype(BF16)
        main_hi = jnp.transpose(dot(spread, scale_hi) * chosen).astype(BF16)
        main_lo = jnp.transpose(dot(spread, scale_lo) * chosen).astype(BF16)
    chosen_extra, extra_hi, extra_lo = [], [], []
    for j in range(extra):
        takes = jnp.where(
            jnp.logical_and(hits > 0.5, jnp.abs(place - (main + j)) < 0.5), 1.0, 0.0
        )
        chosen_extra.append(takes.astype(BF16))
        extra_hi.append(jnp.transpose(scale_hi.astype(F32) * takes).astype(BF16))
        extra_lo.append(jnp.transpose(scale_lo.astype(F32) * takes).astype(BF16))

    pl.semaphore_wait(barrier, n_ep * n_tp - 1)

    def exchange(buffer, k):
        copies = []
        for shift in range(1, n_tp):
            copies.append(
                remote(
                    buffer.at[tp],
                    buffer.at[tp],
                    pair_send.at[k, shift],
                    pair_recv.at[k, shift],
                    {"tp": lax.rem(tp + shift, n_tp)},
                )
            )
            copies[-1].start()
        return copies

    tok_all[tp] = tokens[...]
    for copy in exchange(tok_all, 0):
        copy.wait()

    def as_row(gain):
        return gain[...].astype(F32).reshape(1, gain.shape[0])

    def norm(pieces, gain):
        wide = jnp.concatenate(pieces, axis=1)
        factor = lax.rsqrt(jnp.sum(wide * wide, axis=1, keepdims=True) / width + EPS)
        return (wide * factor * as_row(gain)).astype(BF16)

    token_parts = [tok_all[t].astype(F32) for t in range(n_tp)]
    normed = norm(token_parts, norm_gain)

    for i in range(4):
        loads[i].wait()
    gate_rows = dot(normed, proj_gate[...]).astype(BF16)
    input_rows = dot(normed, proj_input[...]).astype(BF16)
    write_rows = dot(normed, proj_write[...]).astype(BF16)
    read_rows = dot(normed, proj_read[...]).astype(BF16)
    step_all = lax.dot_general(
        normed, proj_step[...], (((1,), (1,)), ((), ())), preferred_element_type=F32
    )

    def conv(window, newest, taps, result):
        old = [window[i] for i in range(window.shape[0])] + [newest]
        lines = [line.astype(F32) for line in old]
        tap = taps[...].astype(F32)
        total = lines[0] * tap[0:1, :]
        for i in range(1, len(lines)):
            total = total + lines[i] * tap[i : i + 1, :]
        for i in range(1, len(lines)):
            result[i - 1] = old[i]
        return silu(total)

    input_conv = conv(input_window, input_rows, taps_input, new_input_window)
    write_conv = conv(write_window, write_rows, taps_write, new_write_window)
    read_conv = conv(read_window, read_rows, taps_read, new_read_window)

    heads_dev = state.shape[1]
    groups_dev = write_conv.shape[1] // STATE
    per_group = heads_dev // groups_dev
    head_lane = lax.broadcasted_iota(jnp.int32, step_all.shape, 1)
    loads[4].wait()
    row_lane = lax.broadcasted_iota(jnp.int32, (HEAD_DIM, rows), 1)
    readouts = []
    for h in range(heads_dev):
        at = tp * heads_dev + h
        raw = jnp.sum(jnp.where(head_lane == at, step_all, 0.0), axis=1, keepdims=True)
        biased = raw + step_bias[at]
        size = jnp.maximum(biased, 0.0) + jnp.log1p(jnp.exp(-jnp.abs(biased)))
        decay = jnp.exp(-size * decay_rate[at])
        head_in = input_conv[:, h * HEAD_DIM : (h + 1) * HEAD_DIM]
        scaled = jnp.transpose(size * head_in)
        g = h // per_group
        write = write_conv[:, g * STATE : (g + 1) * STATE]
        read = read_conv[:, g * STATE : (g + 1) * STATE]
        columns = jnp.zeros((HEAD_DIM, rows), F32)
        for b in range(rows):
            fresh = decay[b : b + 1, :] * state[b, h] + scaled[:, b : b + 1] * write[b : b + 1, :]
            new_state[b, h] = fresh
            column = jnp.sum(fresh * read[b : b + 1, :], axis=1, keepdims=True)
            columns = jnp.where(row_lane == b, column, columns)
        readouts.append(jnp.transpose(columns) + skip_gain[at] * head_in)
    keep = pltpu.make_async_copy(new_state, new_state_hbm, state_sem)
    keep.start()
    gated = jnp.concatenate(readouts, axis=1) * silu(gate_rows.astype(F32))
    span = gated.shape[1] // groups_dev
    grouped = []
    for g in range(groups_dev):
        piece = gated[:, g * span : (g + 1) * span]
        grouped.append(
            piece * lax.rsqrt(jnp.mean(piece * piece, axis=1, keepdims=True) + EPS)
        )
    mixer_rows = (jnp.concatenate(grouped, axis=1) * as_row(out_gain)).astype(BF16)
    loads[5].wait()
    part_all[tp] = dot(mixer_rows, proj_out[...]).astype(BF16)
    for copy in exchange(part_all, 1):
        copy.wait()

    mixed = part_all[0].astype(F32)
    for t in range(1, n_tp):
        mixed = mixed + part_all[t].astype(F32)
    hidden_parts = []
    for t in range(n_tp):
        part = (token_parts[t] + mixed[:, t * quarter : (t + 1) * quarter]).astype(BF16)
        hid_all[t] = part
        hidden_parts.append(part.astype(F32))
    normed_ffn = norm(hidden_parts, ffn_gain)

    if main:
        send_main[...] = dot(chosen_main, normed_ffn).astype(BF16).reshape(send_main.shape)
    for j in range(extra):
        send_extra[j] = dot(chosen_extra[j], normed_ffn)[:, None, :]

    def dispatch(step, carry):
        peer = lax.rem(ep + step, n_ep)
        if main:
            remote(
                send_main.at[peer], recv_main.at[ep], a2a_send.at[0], a2a_recv.at[0], {"ep": peer}
            ).start()
        for j in range(extra):
            remote(
                send_extra.at[j, peer],
                recv_extra.at[j, ep],
                a2a_send.at[1],
                a2a_recv.at[1],
                {"ep": peer},
            ).start()
        return carry

    lax.fori_loop(1, n_ep, dispatch, 0)
    if main:
        pltpu.make_async_copy(send_main.at[ep], recv_main.at[ep], a2a_recv.at[0]).start()
    for j in range(extra):
        pltpu.make_async_copy(send_extra.at[j, ep], recv_extra.at[j, ep], a2a_recv.at[1]).start()

    for i in range(6, 9):
        loads[i].wait()
    dense_hidden = (
        silu(dot(normed_ffn, dense_gate[...])) * dot(normed_ffn, dense_up[...])
    ).astype(BF16)
    for t in range(n_tp):
        dense_send[t] = lax.dot_general(
            dense_hidden,
            dense_down[t * quarter : (t + 1) * quarter, :],
            (((1,), (1,)), ((), ())),
            preferred_element_type=F32,
        ).astype(BF16)
    dense_copies = []
    for shift in range(1, n_tp):
        there = lax.rem(tp + shift, n_tp)
        dense_copies.append(
            remote(
                dense_send.at[there],
                dense_recv.at[tp],
                pair_send.at[2, shift],
                pair_recv.at[2, shift],
                {"tp": there},
            )
        )
        dense_copies[-1].start()
    logit = jnp.sum(normed_ffn.astype(F32) * as_row(branch_gate), axis=1, keepdims=True)
    branch = 1.0 / (1.0 + jnp.exp(-logit))

    for i in range(9, 12):
        loads[i].wait()
    arrived = []
    if main:
        drain(recv_main, a2a_recv.at[0])
        arrived.append(recv_main[...].reshape(n_ep * main, width))
    if extra:
        drain(recv_extra, a2a_recv.at[1])
        for j in range(extra):
            arrived.append(recv_extra[j].reshape(n_ep, width).astype(BF16))
    arrived = jnp.concatenate(arrived, axis=0) if len(arrived) > 1 else arrived[0]
    hidden = (silu(dot(arrived, expert_gate[0])) * dot(arrived, expert_up[0])).astype(BF16)
    for t in range(n_tp):
        produced = dot(hidden, expert_down[0, :, t * quarter : (t + 1) * quarter])
        if main:
            back_main[t] = produced[: n_ep * main].astype(BF16).reshape(back_main.shape[1:])
        for j in range(extra):
            start = n_ep * (main + j)
            back_extra[j, t] = produced[start : start + n_ep][:, None, :]

    def give_back(step, carry):
        peer = lax.rem(ep + step, n_ep)
        for shift in range(n_tp):
            there = lax.rem(tp + shift, n_tp)

            def go():
                if main:
                    remote(
                        back_main.at[there, peer],
                        ret_main.at[tp, ep],
                        a2a_send.at[2],
                        a2a_recv.at[2],
                        {"ep": peer, "tp": there},
                    ).start()
                for j in range(extra):
                    remote(
                        back_extra.at[j, there, peer],
                        ret_extra.at[j, tp, ep],
                        a2a_send.at[3],
                        a2a_recv.at[3],
                        {"ep": peer, "tp": there},
                    ).start()

            if shift == 0:
                pl.when(step > 0)(go)
            else:
                go()
        return carry

    lax.fori_loop(0, n_ep, give_back, 0)
    if main:
        pltpu.make_async_copy(back_main.at[tp, ep], ret_main.at[tp, ep], a2a_recv.at[2]).start()
    for j in range(extra):
        pltpu.make_async_copy(
            back_extra.at[j, tp, ep], ret_extra.at[j, tp, ep], a2a_recv.at[3]
        ).start()

    for copy in dense_copies:
        copy.wait()
    dense_sum = dense_send[tp].astype(F32)
    for shift in range(1, n_tp):
        dense_sum = dense_sum + dense_recv[lax.rem(tp + shift, n_tp)].astype(F32)
    total = hid_all[tp].astype(F32) + branch * dense_sum

    if main:
        drain(ret_main, a2a_recv.at[2])
        for t in range(n_tp):
            back = ret_main[t].reshape(n_ep * main, quarter)
            total = total + dot(main_hi, back) + dot(main_lo, back)
    if extra:
        drain(ret_extra, a2a_recv.at[3])
        for j in range(extra):
            for t in range(n_tp):
                back = ret_extra[j, t].reshape(n_ep, quarter).astype(BF16)
                total = total + dot(extra_hi[j], back) + dot(extra_lo[j], back)
    new_hidden[...] = total.astype(BF16)

    def left(step, carry):
        if main:
            drain(send_main.at[0], a2a_send.at[0])
        for j in range(extra):
            drain(send_extra.at[j, 0], a2a_send.at[1])
        return carry

    lax.fori_loop(1, n_ep, left, 0)

    def left_back(step, carry):
        if main:
            drain(back_main.at[0, 0], a2a_send.at[2])
        for j in range(extra):
            drain(back_extra.at[j, 0, 0], a2a_send.at[3])
        return carry

    lax.fori_loop(1, n_ep * n_tp, left_back, 0)
    keep.wait()


def hand_over(
    hidden,
    state,
    input_window,
    write_window,
    read_window,
    new_hidden,
    new_state,
    new_input_window,
    new_write_window,
    new_read_window,
    held,
    in_sems,
    out_sems,
):
    size = held.shape[0] // PIECES
    ins, outs = [], []
    for i in range(PIECES):
        piece = pl.ds(i * size, size)
        ins.append(pltpu.make_async_copy(state.at[piece], held.at[piece], in_sems.at[i]))
        outs.append(pltpu.make_async_copy(held.at[piece], new_state.at[piece], out_sems.at[i]))
        ins[-1].start()
    new_hidden[...] = hidden[...]
    new_input_window[...] = input_window[...]
    new_write_window[...] = write_window[...]
    new_read_window[...] = read_window[...]
    for i in range(PIECES):
        ins[i].wait()
        outs[i].start()
    for copy in outs:
        copy.wait()


def local(
    n_ep,
    n_tp,
    tokens,
    input_window,
    write_window,
    read_window,
    ssm_state,
    norm_gain,
    proj_gate,
    proj_input,
    proj_write,
    proj_read,
    proj_step,
    taps_input,
    taps_write,
    taps_read,
    step_bias,
    decay_rate,
    skip_gain,
    out_gain,
    proj_out,
    ffn_gain,
    expert_ids,
    expert_weights,
    expert_gate,
    expert_up,
    expert_down,
    dense_gate,
    dense_up,
    dense_down,
    branch_gate,
):
    rows, quarter = tokens.shape
    width = norm_gain.shape[0]
    top_count = expert_ids.shape[1]
    capacity = min(rows, max(2, (3 * rows * top_count + 2 * n_ep - 1) // (2 * n_ep)))
    main = capacity // LANES * LANES
    extra = capacity - main
    held = max(main, LANES)
    spare = max(extra, 1)
    vmem = pl.BlockSpec(memory_space=pltpu.VMEM)
    smem = pl.BlockSpec(memory_space=pltpu.SMEM)
    hbm = pl.BlockSpec(memory_space=pl.ANY)
    streamed = (
        proj_gate,
        proj_input,
        proj_write,
        proj_read,
        proj_out,
        expert_gate,
        expert_up,
        expert_down,
        dense_gate,
        dense_up,
        dense_down,
        ssm_state,
    )
    input_window = input_window.transpose(1, 0, 2)
    write_window = write_window.transpose(1, 0, 2)
    read_window = read_window.transpose(1, 0, 2)
    shape_of = lambda a: jax.ShapeDtypeStruct(a.shape, a.dtype)
    results = pl.pallas_call(
        functools.partial(kernel, n_ep, n_tp, capacity),
        out_shape=(
            shape_of(tokens),
            shape_of(ssm_state),
            shape_of(input_window),
            shape_of(write_window),
            shape_of(read_window),
        ),
        in_specs=[vmem] * 4
        + [hbm]
        + [vmem] * 4
        + [hbm] * 4
        + [vmem] * 4
        + [smem] * 3
        + [hbm, vmem, vmem]
        + [hbm] * 6,
        out_specs=(vmem, hbm, vmem, vmem, vmem),
        scratch_shapes=[pltpu.VMEM(a.shape, a.dtype) for a in streamed]
        + [
            pltpu.VMEM(ssm_state.shape, F32),
            pltpu.VMEM((n_tp, rows, quarter), BF16),
            pltpu.VMEM((n_tp, rows, width), BF16),
            pltpu.VMEM((n_tp, rows, quarter), BF16),
            pltpu.VMEM((n_ep, held, width), BF16),
            pltpu.VMEM((n_ep, held, width), BF16),
            pltpu.VMEM((spare, n_ep, 1, width), F32),
            pltpu.VMEM((spare, n_ep, 1, width), F32),
            pltpu.VMEM((n_tp, n_ep, held, quarter), BF16),
            pltpu.VMEM((n_tp, n_ep, held, quarter), BF16),
            pltpu.VMEM((spare, n_tp, n_ep, 1, quarter), F32),
            pltpu.VMEM((spare, n_tp, n_ep, 1, quarter), F32),
            pltpu.VMEM((n_tp, rows, quarter), BF16),
            pltpu.VMEM((n_tp, rows, quarter), BF16),
            pltpu.SemaphoreType.DMA((12,)),
            pltpu.SemaphoreType.DMA,
            pltpu.SemaphoreType.DMA((3, n_tp)),
            pltpu.SemaphoreType.DMA((3, n_tp)),
            pltpu.SemaphoreType.DMA((4,)),
            pltpu.SemaphoreType.DMA((4,)),
        ],
        compiler_params=pltpu.CompilerParams(
            collective_id=0, has_side_effects=True, vmem_limit_bytes=60 * 1024 * 1024
        ),
    )(
        tokens,
        input_window,
        write_window,
        read_window,
        ssm_state,
        norm_gain,
        ffn_gain,
        branch_gate,
        out_gain,
        proj_gate,
        proj_input,
        proj_write,
        proj_read,
        proj_step.T,
        taps_input,
        taps_write,
        taps_read,
        step_bias,
        decay_rate,
        skip_gain,
        proj_out,
        expert_ids.T,
        expert_weights.T,
        expert_gate,
        expert_up,
        expert_down,
        dense_gate,
        dense_up,
        dense_down,
    )
    outputs = pl.pallas_call(
        hand_over,
        out_shape=tuple(shape_of(r) for r in results),
        in_specs=[vmem, hbm, vmem, vmem, vmem],
        out_specs=(vmem, hbm, vmem, vmem, vmem),
        scratch_shapes=[
            pltpu.VMEM(ssm_state.shape, F32),
            pltpu.SemaphoreType.DMA((PIECES,)),
            pltpu.SemaphoreType.DMA((PIECES,)),
        ],
    )(*results)
    return (
        outputs[0],
        outputs[1],
        outputs[2].transpose(1, 0, 2),
        outputs[3].transpose(1, 0, 2),
        outputs[4].transpose(1, 0, 2),
    )


def solution(mesh):
    in_specs = (
        P("ep", "tp"),
        P("ep", None, "tp"),
        P("ep", None, "tp"),
        P("ep", None, "tp"),
        P("ep", "tp", None, None),
        P(),
        P(None, "tp"),
        P(None, "tp"),
        P(None, "tp"),
        P(None, "tp"),
        P(),
        P(None, "tp"),
        P(None, "tp"),
        P(None, "tp"),
        P(),
        P(),
        P(),
        P("tp"),
        P("tp", None),
        P(),
        P("ep", None),
        P("ep", None),
        P("ep", None, "tp"),
        P("ep", None, "tp"),
        P("ep", "tp", None),
        P(None, "tp"),
        P(None, "tp"),
        P(None, "tp"),
        P(),
    )
    out_specs = (
        P("ep", "tp"),
        P("ep", "tp", None, None),
        P("ep", None, "tp"),
        P("ep", None, "tp"),
        P("ep", None, "tp"),
    )
    step = functools.partial(local, mesh.shape["ep"], mesh.shape["tp"])
    return jax.shard_map(step, mesh=mesh, in_specs=in_specs, out_specs=out_specs, check_vma=False)
```
